32 devices in a mesh: sp: 8 (over z, x), tp: 4 (over y, core).
Axes of the slice: x: 2, y: 2, z: 4, core: 2. Of those that a mesh axis runs over, the one named last changes fastest.
Arguments:
- query: bfloat16 [2048, 1024], P('sp', 'tp'), may hold values from -6 to 6
- forget_logits: bfloat16 [2048, 1024], P('sp', 'tp'), may hold values from -5.5 to 5.5
- written_values: bfloat16 [2048, 1024], P('sp', 'tp'), may hold values from -6 to 6
- output_gate_logits: bfloat16 [2048, 1024], P('sp', 'tp'), may hold values from -6 to 6
- forget_floor_gap: float32 [1024], P('tp'), may hold values from 0 to 0.08
- extra_log_decay: float32 [2048, 1024], P('sp', 'tp'), may hold values from -0.7 to 0
- head_norm_gain: float32 [128], replicated, may hold values from 0.1 to 1.9
- output_weight: bfloat16 [1024, 2048], P('tp'), may hold values from -0.1875 to 0.1875
- residual: bfloat16 [2048, 2048], P(('sp', 'tp')), may hold values from -6 to 6
- mixer_norm_gain: float32 [2048], replicated, may hold values from 0.1 to 1.9
- mixer_up_weight: bfloat16 [2048, 8192], P('sp', 'tp'), may hold values from -0.125 to 0.125
- mixer_down_weight: bfloat16 [8192, 2048], P(('tp', 'sp')), may hold values from -0.0625 to 0.0625
Outputs:
- layer_out: bfloat16 [2048, 2048], P(('sp', 'tp'))
The draws below stay inside these ranges and needn't reach their ends.
All inputs are finite; a program needn't handle non-finite values.
Results may differ from the reference program's by a relative error of at most 0.015.
Values may be sent and summed in bfloat16 or wider, within the bound.
A program may use at most 128 MiB of HBM per device.

```python
import jax
import jax.numpy as jnp
from jax import lax

D = 2048
FF = 8192
HEADS = 8
HEAD_K = 128
HEAD_V = 128
BLOCK = 64
TOK_DEV = 256
WIDTH = 1024
SEQ = 2048
N_SP = 8


def draw_forget_logits(key, part):
    noise_key, offset_key = jax.random.split(key)
    jitter = jnp.clip(jax.random.normal(noise_key, (SEQ, WIDTH), jnp.float32), -4.0, 4.0)
    offsets = jax.random.uniform(offset_key, (SEQ // TOK_DEV, 1, 1), jnp.float32, -1.5, 1.5)
    shifted = jitter.reshape(SEQ // TOK_DEV, TOK_DEV, WIDTH) + offsets
    return shifted.reshape(SEQ, WIDTH).astype(jnp.bfloat16)


def draw_forget_floor_gap(key, part):
    choose_key, slow_key, fast_key = jax.random.split(key, 3)
    slow_share = 0.5
    slow_head = jax.random.uniform(choose_key, (HEADS, 1), jnp.float32) < slow_share
    slow_gap = jnp.exp(jax.random.uniform(slow_key, (HEADS, HEAD_K), jnp.float32, jnp.log(0.2 / SEQ), jnp.log(1.0 / SEQ)))
    fast_gap = jnp.exp(jax.random.uniform(fast_key, (HEADS, HEAD_K), jnp.float32, jnp.log(0.02), jnp.log(0.08)))
    return jnp.where(slow_head, slow_gap, fast_gap).reshape(WIDTH).astype(jnp.float32)


def draw_extra_log_decay(key, part):
    place_key, level_key = jax.random.split(key)
    places = jax.random.randint(place_key, (3,), 0, SEQ)
    levels = jnp.log(jax.random.uniform(level_key, (3, WIDTH), jnp.float32, 0.5, 0.8))
    positions = jnp.arange(SEQ)[:, None]
    summed = jnp.zeros((SEQ, WIDTH), jnp.float32)
    for number in range(3):
        summed = summed + jnp.where(positions == places[number], levels[number][None, :], 0.0)
    return summed


def shard_levels(key, dims, pieces, low, top_value):
    level = 1.0
    for axis_at, parts in pieces:
        steps = jax.random.uniform(jax.random.fold_in(jax.random.fold_in(key, 6), axis_at), (parts,), jnp.float32, low / len(pieces), top_value / len(pieces))
        level = level * jnp.repeat(jnp.exp(steps), dims[axis_at] // parts).reshape((-1,) + (1,) * (len(dims) - 1 - axis_at))
    return level


def centred(key, dims, scale, limit, cuts=(), kind=jnp.bfloat16):
    result = scale * jax.random.normal(key, dims, jnp.float32)
    if cuts:
        result = result * shard_levels(key, dims, cuts, -0.22, 0.18)
    return jnp.clip(result, -limit, limit).astype(kind)


def setup_inputs(seed: int = 0) -> dict:
    streams_of = jax.random.split(jax.random.key(seed), 13)
    query = centred(streams_of[0], (SEQ, WIDTH), 1.0, 6.0, ((0, 8), (1, 4)))
    forget_logits = draw_forget_logits(jax.random.fold_in(streams_of[12], 71), 0)
    written_values = centred(streams_of[2], (SEQ, WIDTH), 1.0, 6.0, ((0, 8), (1, 4)))
    output_gate_logits = centred(streams_of[3], (SEQ, WIDTH), 1.0, 6.0, ((0, 8), (1, 4)))
    forget_floor_gap = draw_forget_floor_gap(jax.random.fold_in(streams_of[12], 71), 0)
    extra_log_decay = draw_extra_log_decay(jax.random.fold_in(streams_of[12], 71), 0)
    head_norm_gain = jnp.clip(1.0 + 0.18 * jax.random.normal(streams_of[6], (HEAD_V,), jnp.float32), 0.1, 1.9)
    output_weight = centred(streams_of[7], (WIDTH, D), WIDTH ** -0.5, 0.1875, ((0, 4),))
    residual = centred(streams_of[8], (SEQ, D), 1.0, 6.0, ((0, 32),))
    mixer_norm_gain = jnp.clip(1.0 + 0.18 * jax.random.normal(streams_of[9], (D,), jnp.float32), 0.1, 1.9)
    mixer_up_weight = centred(streams_of[10], (D, FF), D ** -0.5, 0.125, ((0, 8), (1, 4)))
    mixer_down_weight = centred(streams_of[11], (FF, D), FF ** -0.5, 0.0625, ((0, 32),))
    return {"query": query, "forget_logits": forget_logits, "written_values": written_values, "output_gate_logits": output_gate_logits, "forget_floor_gap": forget_floor_gap, "extra_log_decay": extra_log_decay, "head_norm_gain": head_norm_gain, "output_weight": output_weight, "residual": residual, "mixer_norm_gain": mixer_norm_gain, "mixer_up_weight": mixer_up_weight, "mixer_down_weight": mixer_down_weight}


norm_eps = 1e-06
highest_precision = lax.Precision.HIGHEST

def block_update(carry_forward_state, block_inputs):
    query_rows_block, gate_rows_block, value_rows_block, log_block = block_inputs
    cumulative_log = jnp.cumsum(log_block, axis=1)
    length = query_rows_block.shape[1]
    causal = jnp.arange(length)[:, None] >= jnp.arange(length)[None, :]
    across_blocks = jnp.einsum('dcj,djw->dcw', query_rows_block * jnp.exp(cumulative_log), carry_forward_state, precision=highest_precision)
    spread = cumulative_log[:, :, None, :] - cumulative_log[:, None, :, :]
    decay_table = jnp.exp(jnp.where(causal[None, :, :, None], spread, -jnp.inf))
    scores = jnp.einsum('htk,hsk,htsk->hts', query_rows_block, gate_rows_block, decay_table, precision=highest_precision)
    within = jnp.einsum('hts,hsv->htv', scores, value_rows_block, precision=highest_precision)
    final_log_total = cumulative_log[:, -1:, :]
    updated_state = jnp.exp(final_log_total[:, 0, :])[:, :, None] * carry_forward_state + jnp.einsum('tri,trw->tiw', gate_rows_block * jnp.exp(final_log_total - cumulative_log), value_rows_block, precision=highest_precision)
    return (updated_state, across_blocks + within)

def to_blocks(array, inner):
    length = array.shape[0]
    split_up = array.reshape(length // BLOCK, BLOCK, array.shape[1] // inner, inner)
    return jnp.transpose(split_up, (0, 2, 1, 3))

def from_blocks(blocked):
    joined = jnp.transpose(blocked, (0, 2, 1, 3))
    return joined.reshape(joined.shape[0] * joined.shape[1], joined.shape[2], joined.shape[3])

def prepare_inputs(query, forget_logits, written_values, forget_floor_gap, extra_log_decay):
    input_gate_value = forget_floor_gap[None, :] * jax.nn.sigmoid(-forget_logits.astype(jnp.float32))
    forget_log_rate = jnp.log1p(-input_gate_value) + extra_log_decay
    scaled_values = query.astype(jnp.float32) * HEAD_K ** (-0.5)
    return (scaled_values, input_gate_value, written_values.astype(jnp.float32), forget_log_rate)

def gate_out(recurrent, output_gate_logits, head_norm_gain):
    normal_part = recurrent * lax.rsqrt(lax.optimization_barrier(jnp.mean(recurrent * recurrent, axis=-1, keepdims=True)) + norm_eps)
    gating = jax.nn.silu(output_gate_logits.astype(jnp.float32)).reshape(recurrent.shape)
    mixed = normal_part * head_norm_gain * gating
    return mixed.reshape(recurrent.shape[0], -1).astype(jnp.bfloat16)

def normalize(stream, gain):
    scaled_rows = stream * lax.rsqrt(lax.optimization_barrier(jnp.mean(stream * stream, axis=-1, keepdims=True)) + norm_eps)
    return (scaled_rows * gain).astype(jnp.bfloat16)

def reference(query, forget_logits, written_values, output_gate_logits, forget_floor_gap, extra_log_decay, head_norm_gain, output_weight, residual, mixer_norm_gain, mixer_up_weight, mixer_down_weight):
    scaled_values, input_gate_value, value_rows, forget_log_rate = prepare_inputs(query, forget_logits, written_values, forget_floor_gap, extra_log_decay)
    head_count = query.shape[1] // HEAD_K
    start_state = jnp.zeros((head_count, HEAD_K, HEAD_V), jnp.float32)
    final_state, blocked = lax.scan(block_update, start_state, (to_blocks(scaled_values, HEAD_K), to_blocks(input_gate_value, HEAD_K), to_blocks(value_rows, HEAD_V), to_blocks(forget_log_rate, HEAD_K)))
    mixed = gate_out(from_blocks(blocked), output_gate_logits, head_norm_gain)
    branch = jnp.dot(mixed, output_weight, preferred_element_type=jnp.float32)
    stream = residual.astype(jnp.float32) + branch

    def channel_mix(row_block):
        normed = normalize(row_block, mixer_norm_gain)
        lifted = jnp.dot(normed, mixer_up_weight, preferred_element_type=jnp.float32)
        hidden = jnp.square(jax.nn.relu(lifted)).astype(jnp.bfloat16)
        return (row_block + jnp.dot(hidden, mixer_down_weight, preferred_element_type=jnp.float32)).astype(jnp.bfloat16)
    mapped = lax.map(channel_mix, stream.reshape(N_SP, TOK_DEV, stream.shape[1]))
    return mapped.reshape(stream.shape)
```

```python
import functools

import jax
import jax.numpy as jnp
from jax import lax
from jax.experimental import pallas as pl
from jax.experimental.pallas import tpu as pltpu
from jax.sharding import PartitionSpec as P

HEAD_K = 128
HEAD_V = 128
BLOCK = 64


norm_eps = 1e-06
highest_precision = lax.Precision.HIGHEST


def carried_in(part, axis, combine, identity):
    place = lax.axis_index(axis)
    gathered = jax.tree.map(lambda a: lax.all_gather(a, axis), part)
    state = jax.tree.map(lambda a, e: jnp.zeros_like(a) + jnp.asarray(e, a.dtype), part, identity)

    def one(step, state):
        return combine(
            state, jax.tree.map(lambda a: lax.dynamic_index_in_dim(a, step, 0, False), gathered)
        )

    return lax.fori_loop(0, place, one, state)


def block_update(carry_forward_state, block_inputs):
    query_rows_block, gate_rows_block, value_rows_block, log_block = block_inputs
    cumulative_log = jnp.cumsum(log_block, axis=1)
    length = query_rows_block.shape[1]
    causal = jnp.arange(length)[:, None] >= jnp.arange(length)[None, :]
    across_blocks = jnp.einsum(
        "dcj,djw->dcw",
        query_rows_block * jnp.exp(cumulative_log),
        carry_forward_state,
        precision=highest_precision,
    )
    spread = cumulative_log[:, :, None, :] - cumulative_log[:, None, :, :]
    decay_table = jnp.exp(jnp.where(causal[None, :, :, None], spread, -jnp.inf))
    scores = jnp.einsum(
        "htk,hsk,htsk->hts",
        query_rows_block,
        gate_rows_block,
        decay_table,
        precision=highest_precision,
    )
    within = jnp.einsum("hts,hsv->htv", scores, value_rows_block, precision=highest_precision)
    final_log_total = cumulative_log[:, -1:, :]
    updated_state = jnp.exp(final_log_total[:, 0, :])[
        :, :, None
    ] * carry_forward_state + jnp.einsum(
        "tri,trw->tiw",
        gate_rows_block * jnp.exp(final_log_total - cumulative_log),
        value_rows_block,
        precision=highest_precision,
    )
    return (updated_state, across_blocks + within)


def to_blocks(array, inner):
    length = array.shape[0]
    split_up = array.reshape(length // BLOCK, BLOCK, array.shape[1] // inner, inner)
    return jnp.transpose(split_up, (0, 2, 1, 3))


def from_blocks(blocked):
    joined = jnp.transpose(blocked, (0, 2, 1, 3))
    return joined.reshape(joined.shape[0] * joined.shape[1], joined.shape[2], joined.shape[3])


def prepare_inputs(query, forget_logits, written_values, forget_floor_gap, extra_log_decay):
    input_gate_value = forget_floor_gap[None, :] * jax.nn.sigmoid(
        -forget_logits.astype(jnp.float32)
    )
    forget_log_rate = jnp.log1p(-input_gate_value) + extra_log_decay
    scaled_values = query.astype(jnp.float32) * HEAD_K ** (-0.5)
    return (scaled_values, input_gate_value, written_values.astype(jnp.float32), forget_log_rate)


def gate_out(recurrent, output_gate_logits, head_norm_gain):
    normal_part = recurrent * lax.rsqrt(
        jnp.mean(recurrent * recurrent, axis=-1, keepdims=True) + norm_eps
    )
    gating = jax.nn.silu(output_gate_logits.astype(jnp.float32)).reshape(recurrent.shape)
    mixed = normal_part * head_norm_gain * gating
    return mixed.reshape(recurrent.shape[0], -1).astype(jnp.bfloat16)


def normalize(stream, gain):
    scaled_rows = stream * lax.rsqrt(jnp.mean(stream * stream, axis=-1, keepdims=True) + norm_eps)
    return (scaled_rows * gain).astype(jnp.bfloat16)


def chain_states(earlier, later):
    return (earlier[0] + later[0], jnp.exp(later[0])[:, :, None] * earlier[1] + later[1])


OUTER = 4
LO = 2
MESH = pl.DeviceIdType.MESH


def mixer_kernel(
    sp_size, tp_size,
    mixed_ref, wo_ref, res_ref, gain_ref, up_ref, down_ref, out_ref,
    pbuf, stream, s5, r5, s6, r6, nb, acc, s1, r1, s2, r2, acc2, s3, r3,
    sem5s, sem5r, sem6s, sem6r, zs, zr, hs, hr, ls, lr, ls2, lr2,
    q1s, q1r, q2s, q2r, q3s, q3r,
):
    outer, inner, hi = OUTER, sp_size // OUTER, tp_size // LO
    sp, tp = lax.axis_index("sp"), lax.axis_index("tp")
    o, i = lax.div(sp, inner), lax.rem(sp, inner)
    h, l = lax.div(tp, LO), lax.rem(tp, LO)
    other = 1 - l
    rows, depth = res_ref.shape

    def dev(oo, hh, ll):
        return (oo * inner + i, hh * LO + ll)

    def at_o(k):
        return lax.rem(o + k, outer)

    def from_o(k):
        return lax.rem(o - k + outer, outer)

    def at_h(m):
        return lax.rem(h + m, hi)

    def from_h(m):
        return lax.rem(h - m + hi, hi)

    def rcopy(src, dst, ssem, rsem, device):
        return pltpu.make_async_remote_copy(
            src_ref=src, dst_ref=dst, send_sem=ssem, recv_sem=rsem,
            device_id=device, device_id_type=MESH,
        )

    barrier = pltpu.get_barrier_semaphore()
    peers = [dev(at_o(k), h, l) for k in range(1, outer)]
    peers += [dev(o, at_h(m), l) for m in range(1, hi)] + [dev(o, h, other)]
    for peer in peers:
        pl.semaphore_signal(barrier, inc=1, device_id=peer, device_id_type=MESH)
    pl.semaphore_wait(barrier, len(peers))

    branch = jnp.dot(mixed_ref[...], wo_ref[...], preferred_element_type=jnp.float32)
    pbuf[...] = branch.reshape(tp_size, rows, depth)
    for hh in range(hi):
        s5[hh] = pbuf[hh * LO + other].astype(jnp.bfloat16)
    c5 = rcopy(s5, r5, sem5s, sem5r, dev(o, h, other))
    c5.start()
    c5.wait_recv()
    c6 = []
    for m in range(1, hi):
        to = at_h(m)
        s6[m] = (pbuf[to * LO + l] + r5[to].astype(jnp.float32)).astype(jnp.bfloat16)
        c = rcopy(s6.at[m], r6.at[m], sem6s.at[m], sem6r.at[m], dev(o, to, l))
        c.start()
        c6.append(c)
    total = pbuf[tp] + r5[h].astype(jnp.float32) + res_ref[...].astype(jnp.float32)
    for m in range(1, hi):
        c6[m - 1].wait_recv()
        total = total + r6[m].astype(jnp.float32)
    stream[...] = total
    scale = lax.rsqrt(jnp.mean(total * total, axis=-1, keepdims=True) + norm_eps)
    nb[o, tp] = (total * scale * gain_ref[...]).astype(jnp.bfloat16)

    def z_copy(k):
        return rcopy(nb.at[o, tp], nb.at[o, tp], zs.at[k], zr.at[k], dev(at_o(k), h, l))

    def h_copy(k, m):
        ref = nb.at[from_o(k), tp]
        return rcopy(ref, ref, hs.at[k, m], hr.at[k, m], dev(o, at_h(m), l))

    def l_copy(k):
        ref = nb.at[from_o(k), tp]
        return rcopy(ref, ref, ls.at[k], lr.at[k], dev(o, h, other))

    def l2_copy(k, m):
        ref = nb.at[from_o(k), from_h(m) * LO + l]
        return rcopy(ref, ref, ls2.at[k, m], lr2.at[k, m], dev(o, h, other))

    def s1_copy(k):
        return rcopy(s1.at[k], r1.at[k], q1s.at[k], q1r.at[k], dev(o, h, other))

    def s2_copy(k, m):
        return rcopy(s2.at[k, m], r2.at[k, m], q2s.at[k, m], q2r.at[k, m], dev(o, at_h(m), l))

    def s3_copy(k):
        return rcopy(s3.at[k], r3.at[k], q3s.at[k], q3r.at[k], dev(from_o(k), h, l))

    for k in range(1, outer):
        z_copy(k).start()

    def forward(k):
        for m in range(1, hi):
            h_copy(k, m).start()
        l_copy(k).start()

    forward(0)

    def body(j, carry):
        @pl.when(j + 1 < outer)
        def _():
            z_copy(j + 1).wait_recv()
            forward(j + 1)

        @pl.when(j < outer)
        def _():
            for m in range(1, hi):
                h_copy(j, m).wait_recv()
                l2_copy(j, m).start()
            l_copy(j).wait_recv()
            for m in range(1, hi):
                l2_copy(j, m).wait_recv()
            x = nb[from_o(j)].reshape(tp_size * rows, depth)
            lifted = jnp.dot(x, up_ref[...], preferred_element_type=jnp.float32)
            hidden = jnp.square(jnp.maximum(lifted, 0.0)).astype(jnp.bfloat16)
            part = jnp.dot(hidden, down_ref[...], preferred_element_type=jnp.float32)
            pbuf[...] = part.reshape(tp_size, rows, depth)
            for hh in range(hi):
                s1[j, hh] = pbuf[hh * LO + other].astype(jnp.bfloat16)
            s1_copy(j).start()
            for hh in range(hi):
                acc[j, hh] = pbuf[hh * LO + l]

        @pl.when((j >= 1) & (j < outer + 1))
        def _():
            k = j - 1
            s1_copy(k).wait_recv()
            for m in range(1, hi):
                to = at_h(m)
                s2[k, m] = (acc[k, to] + r1[k, to].astype(jnp.float32)).astype(jnp.bfloat16)
                s2_copy(k, m).start()
            acc2[k] = acc[k, h] + r1[k, h].astype(jnp.float32)

        @pl.when(j >= 2)
        def _():
            k = j - 2
            v = acc2[k]
            for m in range(1, hi):
                s2_copy(k, m).wait_recv()
                v = v + r2[k, m].astype(jnp.float32)
            @pl.when(k == 0)
            def _():
                acc2[0] = v

            @pl.when(k > 0)
            def _():
                s3[k] = v.astype(jnp.bfloat16)
                s3_copy(k).start()

        return carry

    lax.fori_loop(0, outer + 2, body, 0)
    final = stream[...] + acc2[0]
    for k in range(1, outer):
        s3_copy(k).wait_recv()
        final = final + r3[k].astype(jnp.float32)
    out_ref[...] = final.astype(jnp.bfloat16)

    c5.wait_send()
    for c in c6:
        c.wait_send()
    for k in range(outer):
        if k > 0:
            z_copy(k).wait_send()
            s3_copy(k).wait_send()
        l_copy(k).wait_send()
        s1_copy(k).wait_send()
        for m in range(1, hi):
            h_copy(k, m).wait_send()
            l2_copy(k, m).wait_send()
            s2_copy(k, m).wait_send()


def mixer(sp_size, tp_size, mixed, wo, res, gain, up, down):
    rows, depth = res.shape
    hi = tp_size // LO
    f32, b16 = jnp.float32, jnp.bfloat16
    dma = pltpu.SemaphoreType.DMA
    vm = pltpu.VMEM
    O = OUTER
    return pl.pallas_call(
        functools.partial(mixer_kernel, sp_size, tp_size),
        out_shape=jax.ShapeDtypeStruct((rows, depth), b16),
        in_specs=[pl.BlockSpec(memory_space=pltpu.VMEM)] * 6,
        out_specs=pl.BlockSpec(memory_space=pltpu.VMEM),
        scratch_shapes=[
            vm((tp_size, rows, depth), f32),
            vm((rows, depth), f32),
            vm((hi, rows, depth), b16), vm((hi, rows, depth), b16),
            vm((hi, rows, depth), b16), vm((hi, rows, depth), b16),
            vm((O, tp_size, rows, depth), b16),
            vm((O, hi, rows, depth), f32),
            vm((O, hi, rows, depth), b16), vm((O, hi, rows, depth), b16),
            vm((O, hi, rows, depth), b16), vm((O, hi, rows, depth), b16),
            vm((O, rows, depth), f32),
            vm((O, rows, depth), b16), vm((O, rows, depth), b16),
            dma, dma, dma((hi,)), dma((hi,)),
            dma((O,)), dma((O,)), dma((O, hi)), dma((O, hi)),
            dma((O,)), dma((O,)), dma((O, hi)), dma((O, hi)),
            dma((O,)), dma((O,)), dma((O, hi)), dma((O, hi)),
            dma((O,)), dma((O,)),
        ],
        compiler_params=pltpu.CompilerParams(
            collective_id=0, has_side_effects=True, vmem_limit_bytes=60 * 1024 * 1024
        ),
    )(mixed, wo, res, gain.reshape(1, depth), up, down)


def regroup_weights(sp_size, up, down):
    inner = sp_size // OUTER
    inner_groups = [[o * inner + i for i in range(inner)] for o in range(OUTER)]
    down_own = lax.all_gather(down, "sp", axis=0, tiled=True, axis_index_groups=inner_groups)
    depth_part, cols = up.shape
    width = cols // OUTER
    o = lax.div(lax.axis_index("sp"), inner)
    pieces = []
    for k in range(OUTER):
        to = lax.rem(o + k, OUTER)
        piece = lax.dynamic_slice_in_dim(up, to * width, width, 1)
        if k:
            perm = [(s, (s + k * inner) % sp_size) for s in range(sp_size)]
            piece = lax.ppermute(piece, "sp", perm)
        pieces.append(piece)
    stacked = jnp.stack(pieces)
    both = lax.all_gather(stacked, "sp", axis=0, tiled=False, axis_index_groups=inner_groups)
    order = lax.rem(o - jnp.arange(OUTER) + OUTER, OUTER)
    both = jnp.take(both, order, axis=1)
    full = jnp.transpose(both, (1, 0, 2, 3)).reshape(sp_size * depth_part, width)
    return full, down_own


def on_device(
    sp_size,
    tp_size,
    query,
    forget_logits,
    written_values,
    output_gate_logits,
    forget_floor_gap,
    extra_log_decay,
    head_norm_gain,
    output_weight,
    residual,
    mixer_norm_gain,
    mixer_up_weight,
    mixer_down_weight,
):
    scaled_values, input_gate_value, value_rows, forget_log_rate = prepare_inputs(
        query, forget_logits, written_values, forget_floor_gap, extra_log_decay
    )
    row_count, local_width = query.shape
    head_count = local_width // HEAD_K
    start_state = jnp.zeros((head_count, HEAD_K, HEAD_V), jnp.float32)
    local_state, blocked = lax.scan(
        block_update,
        start_state,
        (
            to_blocks(scaled_values, HEAD_K),
            to_blocks(input_gate_value, HEAD_K),
            to_blocks(value_rows, HEAD_V),
            to_blocks(forget_log_rate, HEAD_K),
        ),
    )
    log_total = jnp.sum(forget_log_rate, axis=0).reshape(head_count, HEAD_K)
    arrived_state = carried_in(
        (log_total, local_state),
        "sp",
        chain_states,
        (jnp.zeros_like(log_total), jnp.zeros_like(local_state)),
    )
    running = jnp.cumsum(forget_log_rate, axis=0)
    reached_state = (scaled_values * jnp.exp(running)).reshape(row_count, head_count, HEAD_K)
    carried_over = jnp.einsum(
        "cja,jae->cje", reached_state, arrived_state[1], precision=highest_precision
    )
    mixed = gate_out(from_blocks(blocked) + carried_over, output_gate_logits, head_norm_gain)
    up_own, down_own = regroup_weights(sp_size, mixer_up_weight, mixer_down_weight)
    return mixer(
        sp_size, tp_size, mixed, output_weight, residual, mixer_norm_gain, up_own, down_own
    )


def solution(mesh):
    return jax.shard_map(
        functools.partial(on_device, mesh.shape["sp"], mesh.shape["tp"]),
        mesh=mesh,
        in_specs=(
            P("sp", "tp"),
            P("sp", "tp"),
            P("sp", "tp"),
            P("sp", "tp"),
            P("tp"),
            P("sp", "tp"),
            P(),
            P("tp", None),
            P(("sp", "tp"), None),
            P(),
            P("sp", "tp"),
            P(("tp", "sp"), None),
        ),
        out_specs=P(("sp", "tp"), None),
        check_vma=False,
    )
```

```python
import functools

import jax
import jax.numpy as jnp
from jax import lax
from jax.experimental import pallas as pl
from jax.experimental.pallas import tpu as pltpu
from jax.sharding import PartitionSpec as P

HEAD_K = 128
HEAD_V = 128
BLOCK = 64


norm_eps = 1e-06
highest_precision = lax.Precision.HIGHEST


OUTER = 4
LO = 2
MESH = pl.DeviceIdType.MESH


def layer_kernel(
    sp_size, tp_size,
    q_ref, f_ref, v_ref, g_ref, gap_ref, ex_ref, hg_ref,
    wo_ref, res_ref, gain_ref, upsh_ref, downsh_ref, out_ref,
    upbuf, downbuf, rec, qrun, mixed_ref, ins, int_, outs, outt,
    pbuf, stream, s5, r5, s6, r6, nb, acc, s1, r1, s2, r2, acc2, s3, r3,
    sem5s, sem5r, sem6s, sem6r, zs, zr, hs, hr, ls, lr, ls2, lr2,
    q1s, q1r, q2s, q2r, q3s, q3r,
    wl, wzs, wzr, wxs, wxr, wds, wdr, iss, isr, its, itr, oss, osr, ots, otr,
):
    outer, inner, hi = OUTER, sp_size // OUTER, tp_size // LO
    sp, tp = lax.axis_index("sp"), lax.axis_index("tp")
    o, i = lax.div(sp, inner), lax.rem(sp, inner)
    h, l = lax.div(tp, LO), lax.rem(tp, LO)
    other = 1 - l
    rows, depth = res_ref.shape

    def dev(oo, hh, ll):
        return (oo * inner + i, hh * LO + ll)

    def at_i(j):
        return (o * inner + lax.rem(i + j, inner), tp)

    def at_o(k):
        return lax.rem(o + k, outer)

    def from_o(k):
        return lax.rem(o - k + outer, outer)

    def at_h(m):
        return lax.rem(h + m, hi)

    def from_h(m):
        return lax.rem(h - m + hi, hi)

    def rcopy(src, dst, ssem, rsem, device):
        return pltpu.make_async_remote_copy(
            src_ref=src, dst_ref=dst, send_sem=ssem, recv_sem=rsem,
            device_id=device, device_id_type=MESH,
        )

    barrier = pltpu.get_barrier_semaphore()
    peers = [dev(at_o(k), h, l) for k in range(1, outer)]
    peers += [dev(o, at_h(m), l) for m in range(1, hi)] + [dev(o, h, other)]
    peers += [at_i(j) for j in range(1, inner)]
    for peer in peers:
        pl.semaphore_signal(barrier, inc=1, device_id=peer, device_id_type=MESH)
    pl.semaphore_wait(barrier, len(peers))

    width = upbuf.shape[2]

    def up_piece(to):
        return upsh_ref.at[:, pl.ds(pl.multiple_of(to * width, width), width)]

    def wz_copy(k):
        return rcopy(up_piece(at_o(k)), upbuf.at[sp], wzs.at[k], wzr.at[k], dev(at_o(k), h, l))

    def wx_copy(k, j):
        ref = upbuf.at[from_o(k) * inner + i]
        return rcopy(ref, ref, wxs.at[k, j], wxr.at[k, j], at_i(j))

    def wd_copy(j):
        return rcopy(downsh_ref, downbuf.at[i], wds.at[j], wdr.at[j], at_i(j))

    own_up = pltpu.make_async_copy(up_piece(o), upbuf.at[sp], wl.at[0])
    own_down = pltpu.make_async_copy(downsh_ref, downbuf.at[i], wl.at[1])
    for k in range(1, outer):
        wz_copy(k).start()
    for j in range(1, inner):
        wd_copy(j).start()
    own_up.start()
    own_down.start()

    length = q_ref.shape[0]
    heads = q_ref.shape[1] // HEAD_K
    row_at = lax.broadcasted_iota(jnp.int32, (BLOCK, BLOCK), 0)
    col_at = lax.broadcasted_iota(jnp.int32, (BLOCK, BLOCK), 1)
    causal = row_at >= col_at
    lower = causal.astype(jnp.float32)

    def dot(a, b, dims):
        return lax.dot_general(
            a, b, (dims, ((), ())), precision=highest_precision,
            preferred_element_type=jnp.float32,
        )

    states = [jnp.zeros((HEAD_V, HEAD_K), jnp.float32) for _ in range(heads)]
    before = jnp.zeros((1, q_ref.shape[1]), jnp.float32)
    for b in range(length // BLOCK):
        at = pl.ds(b * BLOCK, BLOCK)
        gate = gap_ref[...] * (1.0 / (1.0 + jnp.exp(f_ref[at, :].astype(jnp.float32))))
        rate = jnp.log1p(-gate) + ex_ref[at, :]
        cum = dot(lower, rate, ((1,), (0,)))
        last = cum[BLOCK - 1 : BLOCK, :]
        qe = q_ref[at, :].astype(jnp.float32) * HEAD_K ** (-0.5) * jnp.exp(cum)
        ke = gate * jnp.exp(-cum)
        kd = gate * jnp.exp(last - cum)
        keep = jnp.exp(last)
        qrun[at, :] = qe * jnp.exp(before)
        before = before + last
        for n in range(heads):
            lane = slice(n * HEAD_K, (n + 1) * HEAD_K)
            val = v_ref[at, lane].astype(jnp.float32)
            scores = dot(qe[:, lane], ke[:, lane], ((1,), (1,)))
            scores = jnp.where(causal, scores, 0.0)
            got = dot(scores, val, ((1,), (0,)))
            if b:
                got = got + dot(qe[:, lane], states[n], ((1,), (1,)))
            rec[at, lane] = got
            fresh = dot(val, kd[:, lane], ((0,), (0,)))
            states[n] = states[n] * keep[:, lane] + fresh

    def is_copy(j):
        return rcopy(ins.at[i], ins.at[i], iss.at[j], isr.at[j], at_i(j))

    def it_copy(j):
        return rcopy(int_.at[i], int_.at[i], its.at[j], itr.at[j], at_i(j))

    def os_copy(k):
        return rcopy(outs.at[o], outs.at[o], oss.at[k], osr.at[k], dev(at_o(k), h, l))

    def ot_copy(k):
        return rcopy(outt.at[o], outt.at[o], ots.at[k], otr.at[k], dev(at_o(k), h, l))

    for n in range(heads):
        ins[i, n] = states[n].astype(jnp.bfloat16)
    int_[i] = jnp.broadcast_to(before, int_.shape[1:])
    for j in range(1, inner):
        is_copy(j).start()
        it_copy(j).start()
    for j in range(1, inner):
        is_copy(j).wait_recv()
        it_copy(j).wait_recv()

    def fold(carry, state_ref, log_ref, at, use):
        logs, parts = carry
        log = log_ref[at][0:1, :]
        keep = jnp.exp(log)
        new = []
        for n in range(heads):
            lane = slice(n * HEAD_K, (n + 1) * HEAD_K)
            step = parts[n] * keep[:, lane] + state_ref[at, n].astype(jnp.float32)
            new.append(step if use is None else jnp.where(use, step, parts[n]))
        both = logs + log
        return (both if use is None else jnp.where(use, both, logs), new)

    nothing = (
        jnp.zeros((1, q_ref.shape[1]), jnp.float32),
        [jnp.zeros((HEAD_V, HEAD_K), jnp.float32) for _ in range(heads)],
    )
    group, inner_part = nothing, nothing
    for j in range(inner):
        group = fold(group, ins, int_, j, None)
        inner_part = fold(inner_part, ins, int_, j, j < i)
    for n in range(heads):
        outs[o, n] = group[1][n].astype(jnp.bfloat16)
    outt[o] = jnp.broadcast_to(group[0], outt.shape[1:])
    for k in range(1, outer):
        os_copy(k).start()
        ot_copy(k).start()
    own_up.wait()
    for k in range(outer):
        if k:
            wz_copy(k).wait_recv()
        for j in range(1, inner):
            wx_copy(k, j).start()
    for k in range(1, outer):
        os_copy(k).wait_recv()
        ot_copy(k).wait_recv()
    arrived = nothing
    for k in range(outer):
        arrived = fold(arrived, outs, outt, k, k < o)
    inner_keep = jnp.exp(inner_part[0])
    for n in range(heads):
        lane = slice(n * HEAD_K, (n + 1) * HEAD_K)
        came = arrived[1][n] * inner_keep[:, lane] + inner_part[1][n]
        out = rec[:, lane] + dot(qrun[:, lane], came, ((1,), (1,)))
        out = out * lax.rsqrt(jnp.mean(out * out, axis=-1, keepdims=True) + norm_eps)
        logit = g_ref[:, lane].astype(jnp.float32)
        gating = logit / (1.0 + jnp.exp(-logit))
        mixed_ref[:, lane] = (out * hg_ref[...] * gating).astype(jnp.bfloat16)

    branch = jnp.dot(mixed_ref[...], wo_ref[...], preferred_element_type=jnp.float32)
    pbuf[...] = branch.reshape(tp_size, rows, depth)
    for hh in range(hi):
        s5[hh] = pbuf[hh * LO + other].astype(jnp.bfloat16)
    c5 = rcopy(s5, r5, sem5s, sem5r, dev(o, h, other))
    c5.start()
    c5.wait_recv()
    c6 = []
    for m in range(1, hi):
        to = at_h(m)
        s6[m] = (pbuf[to * LO + l] + r5[to].astype(jnp.float32)).astype(jnp.bfloat16)
        c = rcopy(s6.at[m], r6.at[m], sem6s.at[m], sem6r.at[m], dev(o, to, l))
        c.start()
        c6.append(c)
    total = pbuf[tp] + r5[h].astype(jnp.float32) + res_ref[...].astype(jnp.float32)
    for m in range(1, hi):
        c6[m - 1].wait_recv()
        total = total + r6[m].astype(jnp.float32)
    stream[...] = total
    scale = lax.rsqrt(jnp.mean(total * total, axis=-1, keepdims=True) + norm_eps)
    nb[o, tp] = (total * scale * gain_ref[...]).astype(jnp.bfloat16)

    def z_copy(k):
        return rcopy(nb.at[o, tp], nb.at[o, tp], zs.at[k], zr.at[k], dev(at_o(k), h, l))

    def h_copy(k, m):
        ref = nb.at[from_o(k), tp]
        return rcopy(ref, ref, hs.at[k, m], hr.at[k, m], dev(o, at_h(m), l))

    def l_copy(k):
        ref = nb.at[from_o(k), tp]
        return rcopy(ref, ref, ls.at[k], lr.at[k], dev(o, h, other))

    def l2_copy(k, m):
        ref = nb.at[from_o(k), from_h(m) * LO + l]
        return rcopy(ref, ref, ls2.at[k, m], lr2.at[k, m], dev(o, h, other))

    def s1_copy(k):
        return rcopy(s1.at[k], r1.at[k], q1s.at[k], q1r.at[k], dev(o, h, other))

    def s2_copy(k, m):
        return rcopy(s2.at[k, m], r2.at[k, m], q2s.at[k, m], q2r.at[k, m], dev(o, at_h(m), l))

    def s3_copy(k):
        return rcopy(s3.at[k], r3.at[k], q3s.at[k], q3r.at[k], dev(from_o(k), h, l))

    for k in range(1, outer):
        z_copy(k).start()

    def forward(k):
        for m in range(1, hi):
            h_copy(k, m).start()
        l_copy(k).start()

    forward(0)
    own_down.wait()
    for j in range(1, inner):
        wd_copy(j).wait_recv()
        for k in range(outer):
            wx_copy(k, j).wait_recv()

    def body(j, carry):
        @pl.when(j + 1 < outer)
        def _():
            z_copy(j + 1).wait_recv()
            forward(j + 1)

        @pl.when(j < outer)
        def _():
            for m in range(1, hi):
                h_copy(j, m).wait_recv()
                l2_copy(j, m).start()
            l_copy(j).wait_recv()
            for m in range(1, hi):
                l2_copy(j, m).wait_recv()
            x = nb[from_o(j)].reshape(tp_size * rows, depth)
            lifted = jnp.dot(x, upbuf[...].reshape(depth, width), preferred_element_type=jnp.float32)
            hidden = jnp.square(jnp.maximum(lifted, 0.0)).astype(jnp.bfloat16)
            part = jnp.dot(hidden, downbuf[...].reshape(width, depth), preferred_element_type=jnp.float32)
            pbuf[...] = part.reshape(tp_size, rows, depth)
            for hh in range(hi):
                s1[j, hh] = pbuf[hh * LO + other].astype(jnp.bfloat16)
            s1_copy(j).start()
            for hh in range(hi):
                acc[j, hh] = pbuf[hh * LO + l]

        @pl.when((j >= 1) & (j < outer + 1))
        def _():
            k = j - 1
            s1_copy(k).wait_recv()
            for m in range(1, hi):
                to = at_h(m)
                s2[k, m] = (acc[k, to] + r1[k, to].astype(jnp.float32)).astype(jnp.bfloat16)
                s2_copy(k, m).start()
            acc2[k] = acc[k, h] + r1[k, h].astype(jnp.float32)

        @pl.when(j >= 2)
        def _():
            k = j - 2
            v = acc2[k]
            for m in range(1, hi):
                s2_copy(k, m).wait_recv()
                v = v + r2[k, m].astype(jnp.float32)
            @pl.when(k == 0)
            def _():
                acc2[0] = v

            @pl.when(k > 0)
            def _():
                s3[k] = v.astype(jnp.bfloat16)
                s3_copy(k).start()

        return carry

    lax.fori_loop(0, outer + 2, body, 0)
    final = stream[...] + acc2[0]
    for k in range(1, outer):
        s3_copy(k).wait_recv()
        final = final + r3[k].astype(jnp.float32)
    out_ref[...] = final.astype(jnp.bfloat16)

    for k in range(1, outer):
        wz_copy(k).wait_send()
        os_copy(k).wait_send()
        ot_copy(k).wait_send()
    for j in range(1, inner):
        wd_copy(j).wait_send()
        is_copy(j).wait_send()
        it_copy(j).wait_send()
        for k in range(outer):
            wx_copy(k, j).wait_send()
    c5.wait_send()
    for c in c6:
        c.wait_send()
    for k in range(outer):
        if k > 0:
            z_copy(k).wait_send()
            s3_copy(k).wait_send()
        l_copy(k).wait_send()
        s1_copy(k).wait_send()
        for m in range(1, hi):
            h_copy(k, m).wait_send()
            l2_copy(k, m).wait_send()
            s2_copy(k, m).wait_send()


def on_device(
    sp_size, tp_size,
    query, forget_logits, written_values, output_gate_logits, forget_floor_gap,
    extra_log_decay, head_norm_gain, output_weight, residual, mixer_norm_gain,
    mixer_up_weight, mixer_down_weight,
):
    rows, depth = residual.shape
    length, wide = query.shape
    heads = wide // HEAD_K
    hi = tp_size // LO
    f32, b16 = jnp.float32, jnp.bfloat16
    dma = pltpu.SemaphoreType.DMA
    vm = pltpu.VMEM
    O = OUTER
    inner = sp_size // O
    part, cols = mixer_up_weight.shape
    width = cols // O
    return pl.pallas_call(
        functools.partial(layer_kernel, sp_size, tp_size),
        out_shape=jax.ShapeDtypeStruct((rows, depth), b16),
        in_specs=[pl.BlockSpec(memory_space=pltpu.VMEM)] * 12,
        out_specs=pl.BlockSpec(memory_space=pltpu.VMEM),
        scratch_shapes=[
            vm((sp_size, part, width), b16), vm((inner,) + mixer_down_weight.shape, b16),
            vm((length, wide), f32), vm((length, wide), f32), vm((length, wide), b16),
            vm((inner, heads, HEAD_V, HEAD_K), b16), vm((inner, 8, wide), f32),
            vm((O, heads, HEAD_V, HEAD_K), b16), vm((O, 8, wide), f32),
            vm((tp_size, rows, depth), f32),
            vm((rows, depth), f32),
            vm((hi, rows, depth), b16), vm((hi, rows, depth), b16),
            vm((hi, rows, depth), b16), vm((hi, rows, depth), b16),
            vm((O, tp_size, rows, depth), b16),
            vm((O, hi, rows, depth), f32),
            vm((O, hi, rows, depth), b16), vm((O, hi, rows, depth), b16),
            vm((O, hi, rows, depth), b16), vm((O, hi, rows, depth), b16),
            vm((O, rows, depth), f32),
            vm((O, rows, depth), b16), vm((O, rows, depth), b16),
            dma, dma, dma((hi,)), dma((hi,)),
            dma((O,)), dma((O,)), dma((O, hi)), dma((O, hi)),
            dma((O,)), dma((O,)), dma((O, hi)), dma((O, hi)),
            dma((O,)), dma((O,)), dma((O, hi)), dma((O, hi)),
            dma((O,)), dma((O,)),
            dma((2,)), dma((O,)), dma((O,)), dma((O, inner)), dma((O, inner)),
            dma((inner,)), dma((inner,)),
            dma((inner,)), dma((inner,)), dma((inner,)), dma((inner,)),
            dma((O,)), dma((O,)), dma((O,)), dma((O,)),
        ],
        compiler_params=pltpu.CompilerParams(
            collective_id=0, has_side_effects=True, vmem_limit_bytes=60 * 1024 * 1024
        ),
    )(
        query, forget_logits, written_values, output_gate_logits,
        forget_floor_gap.reshape(1, wide), extra_log_decay, head_norm_gain.reshape(1, HEAD_V),
        output_weight, residual, mixer_norm_gain.reshape(1, depth),
        mixer_up_weight, mixer_down_weight,
    )


def solution(mesh):
    return jax.shard_map(
        functools.partial(on_device, mesh.shape["sp"], mesh.shape["tp"]),
        mesh=mesh,
        in_specs=(
            P("sp", "tp"),
            P("sp", "tp"),
            P("sp", "tp"),
            P("sp", "tp"),
            P("tp"),
            P("sp", "tp"),
            P(),
            P("tp", None),
            P(("sp", "tp"), None),
            P(),
            P("sp", "tp"),
            P(("tp", "sp"), None),
        ),
        out_specs=P(("sp", "tp"), None),
        check_vma=False,
    )
```

```python
import functools

import jax
import jax.numpy as jnp
from jax import lax
from jax.experimental import pallas as pl
from jax.experimental.pallas import tpu as pltpu
from jax.sharding import PartitionSpec as P

HEAD_K = 128
HEAD_V = 128
BLOCK = 64


norm_eps = 1e-06
highest_precision = lax.Precision.HIGHEST


OUTER = 4
LO = 2
MESH = pl.DeviceIdType.MESH


def layer_kernel(
    sp_size, tp_size,
    q_ref, f_ref, v_ref, g_ref, gap_ref, ex_ref, hg_ref,
    wo_ref, res_ref, gain_ref, upsh_ref, downsh_ref, out_ref,
    upbuf, downbuf, rec, qrun, mixed_ref, ins, int_, outs, outt,
    pbuf, stream, s5, r5, s6, r6, nb, acc, s1, r1, s2, r2, acc2, s3, r3,
    sem5s, sem5r, sem6s, sem6r, zs, zr, hs, hr, ls, lr, ls2, lr2,
    q1s, q1r, q2s, q2r, q3s, q3r,
    wl, wzs, wzr, wxs, wxr, wds, wdr, iss, isr, its, itr, oss, osr, ots, otr,
):
    outer, inner, hi = OUTER, sp_size // OUTER, tp_size // LO
    sp, tp = lax.axis_index("sp"), lax.axis_index("tp")
    o, i = lax.div(sp, inner), lax.rem(sp, inner)
    h, l = lax.div(tp, LO), lax.rem(tp, LO)
    other = 1 - l
    rows, depth = res_ref.shape

    def dev(oo, hh, ll):
        return (oo * inner + i, hh * LO + ll)

    def at_i(j):
        return (o * inner + lax.rem(i + j, inner), tp)

    def at_o(k):
        return lax.rem(o + k, outer)

    def from_o(k):
        return lax.rem(o - k + outer, outer)

    def at_h(m):
        return lax.rem(h + m, hi)

    def from_h(m):
        return lax.rem(h - m + hi, hi)

    def rcopy(src, dst, ssem, rsem, device):
        return pltpu.make_async_remote_copy(
            src_ref=src, dst_ref=dst, send_sem=ssem, recv_sem=rsem,
            device_id=device, device_id_type=MESH,
        )

    barrier = pltpu.get_barrier_semaphore()
    peers = [dev(at_o(k), h, l) for k in range(1, outer)]
    peers += [dev(o, at_h(m), l) for m in range(1, hi)] + [dev(o, h, other)]
    peers += [at_i(j) for j in range(1, inner)]
    for peer in peers:
        pl.semaphore_signal(barrier, inc=1, device_id=peer, device_id_type=MESH)
    pl.semaphore_wait(barrier, len(peers))

    width = upbuf.shape[2]

    def up_piece(to):
        return upsh_ref.at[:, pl.ds(pl.multiple_of(to * width, width), width)]

    def wz_copy(k):
        return rcopy(up_piece(at_o(k)), upbuf.at[sp], wzs.at[k], wzr.at[k], dev(at_o(k), h, l))

    def wx_copy(k, j):
        ref = upbuf.at[from_o(k) * inner + i]
        return rcopy(ref, ref, wxs.at[k, j], wxr.at[k, j], at_i(j))

    half = downsh_ref.shape[0] // 2

    def wd_copy(j, p):
        some = pl.ds(p * half, half)
        return rcopy(
            downsh_ref.at[some], downbuf.at[i, some], wds.at[j, p], wdr.at[j, p], at_i(j)
        )

    own_up = pltpu.make_async_copy(up_piece(o), upbuf.at[sp], wl.at[0])
    own_down = pltpu.make_async_copy(downsh_ref, downbuf.at[i], wl.at[1])
    wz_copy(1).start()
    wz_copy(2).start()
    own_up.start()
    own_down.start()

    length = q_ref.shape[0]
    heads = q_ref.shape[1] // HEAD_K
    row_at = lax.broadcasted_iota(jnp.int32, (BLOCK, BLOCK), 0)
    col_at = lax.broadcasted_iota(jnp.int32, (BLOCK, BLOCK), 1)
    causal = row_at >= col_at
    lower = causal.astype(jnp.float32)

    def dot(a, b, dims):
        return lax.dot_general(
            a, b, (dims, ((), ())), precision=highest_precision,
            preferred_element_type=jnp.float32,
        )

    states = [jnp.zeros((HEAD_V, HEAD_K), jnp.float32) for _ in range(heads)]
    before = jnp.zeros((1, q_ref.shape[1]), jnp.float32)
    for b in range(length // BLOCK):
        at = pl.ds(b * BLOCK, BLOCK)
        gate = gap_ref[...] * (1.0 / (1.0 + jnp.exp(f_ref[at, :].astype(jnp.float32))))
        rate = jnp.log1p(-gate) + ex_ref[at, :]
        cum = dot(lower, rate, ((1,), (0,)))
        last = cum[BLOCK - 1 : BLOCK, :]
        qe = q_ref[at, :].astype(jnp.float32) * HEAD_K ** (-0.5) * jnp.exp(cum)
        ke = gate * jnp.exp(-cum)
        kd = gate * jnp.exp(last - cum)
        keep = jnp.exp(last)
        qrun[at, :] = qe * jnp.exp(before)
        before = before + last
        for n in range(heads):
            lane = slice(n * HEAD_K, (n + 1) * HEAD_K)
            val = v_ref[at, lane].astype(jnp.float32)
            scores = dot(qe[:, lane], ke[:, lane], ((1,), (1,)))
            scores = jnp.where(causal, scores, 0.0)
            got = dot(scores, val, ((1,), (0,)))
            if b:
                got = got + dot(qe[:, lane], states[n], ((1,), (1,)))
            rec[at, lane] = got
            fresh = dot(val, kd[:, lane], ((0,), (0,)))
            states[n] = states[n] * keep[:, lane] + fresh

    def is_copy(j):
        return rcopy(ins.at[i], ins.at[i], iss.at[j], isr.at[j], at_i(j))

    def it_copy(j):
        return rcopy(int_.at[i], int_.at[i], its.at[j], itr.at[j], at_i(j))

    def os_copy(k):
        return rcopy(outs.at[o], outs.at[o], oss.at[k], osr.at[k], dev(at_o(k), h, l))

    def ot_copy(k):
        return rcopy(outt.at[o], outt.at[o], ots.at[k], otr.at[k], dev(at_o(k), h, l))

    for n in range(heads):
        ins[i, n] = states[n].astype(jnp.bfloat16)
    int_[i] = jnp.broadcast_to(before, int_.shape[1:])
    for j in range(1, inner):
        is_copy(j).start()
        it_copy(j).start()
    for j in range(1, inner):
        wd_copy(j, 1).start()
    for j in range(1, inner):
        wd_copy(j, 0).start()
    for j in range(1, inner):
        is_copy(j).wait_recv()
        it_copy(j).wait_recv()

    def fold(carry, state_ref, log_ref, at, use):
        logs, parts = carry
        log = log_ref[at][0:1, :]
        keep = jnp.exp(log)
        new = []
        for n in range(heads):
            lane = slice(n * HEAD_K, (n + 1) * HEAD_K)
            step = parts[n] * keep[:, lane] + state_ref[at, n].astype(jnp.float32)
            new.append(step if use is None else jnp.where(use, step, parts[n]))
        both = logs + log
        return (both if use is None else jnp.where(use, both, logs), new)

    nothing = (
        jnp.zeros((1, q_ref.shape[1]), jnp.float32),
        [jnp.zeros((HEAD_V, HEAD_K), jnp.float32) for _ in range(heads)],
    )
    group, inner_part = nothing, nothing
    for j in range(inner):
        group = fold(group, ins, int_, j, None)
        inner_part = fold(inner_part, ins, int_, j, j < i)
    for n in range(heads):
        outs[o, n] = group[1][n].astype(jnp.bfloat16)
    outt[o] = jnp.broadcast_to(group[0], outt.shape[1:])
    for k in range(1, outer):
        os_copy(k).start()
        ot_copy(k).start()
    for k in range(3, outer):
        wz_copy(k).start()
    own_up.wait()
    wz_copy(1).wait_recv()
    for k in range(2):
        for j in range(1, inner):
            wx_copy(k, j).start()
    for k in range(1, outer):
        os_copy(k).wait_recv()
        ot_copy(k).wait_recv()
    arrived = nothing
    for k in range(outer):
        arrived = fold(arrived, outs, outt, k, k < o)
    inner_keep = jnp.exp(inner_part[0])
    for n in range(heads):
        lane = slice(n * HEAD_K, (n + 1) * HEAD_K)
        came = arrived[1][n] * inner_keep[:, lane] + inner_part[1][n]
        out = rec[:, lane] + dot(qrun[:, lane], came, ((1,), (1,)))
        out = out * lax.rsqrt(jnp.mean(out * out, axis=-1, keepdims=True) + norm_eps)
        logit = g_ref[:, lane].astype(jnp.float32)
        gating = logit / (1.0 + jnp.exp(-logit))
        mixed_ref[:, lane] = (out * hg_ref[...] * gating).astype(jnp.bfloat16)

    branch = jnp.dot(mixed_ref[...], wo_ref[...], preferred_element_type=jnp.float32)
    pbuf[...] = branch.reshape(tp_size, rows, depth)
    for hh in range(hi):
        s5[hh] = pbuf[hh * LO + other].astype(jnp.bfloat16)
    c5 = rcopy(s5, r5, sem5s, sem5r, dev(o, h, other))
    c5.start()
    c5.wait_recv()
    c6 = []
    for m in range(1, hi):
        to = at_h(m)
        s6[m] = (pbuf[to * LO + l] + r5[to].astype(jnp.float32)).astype(jnp.bfloat16)
        c = rcopy(s6.at[m], r6.at[m], sem6s.at[m], sem6r.at[m], dev(o, to, l))
        c.start()
        c6.append(c)
    total = pbuf[tp] + r5[h].astype(jnp.float32) + res_ref[...].astype(jnp.float32)
    for m in range(1, hi):
        c6[m - 1].wait_recv()
        total = total + r6[m].astype(jnp.float32)
    stream[...] = total
    scale = lax.rsqrt(jnp.mean(total * total, axis=-1, keepdims=True) + norm_eps)
    nb[o, tp] = (total * scale * gain_ref[...]).astype(jnp.bfloat16)

    def z_copy(k):
        return rcopy(nb.at[o, tp], nb.at[o, tp], zs.at[k], zr.at[k], dev(at_o(k), h, l))

    def h_copy(k, m):
        ref = nb.at[from_o(k), tp]
        return rcopy(ref, ref, hs.at[k, m], hr.at[k, m], dev(o, at_h(m), l))

    def l_copy(k):
        ref = nb.at[from_o(k), tp]
        return rcopy(ref, ref, ls.at[k], lr.at[k], dev(o, h, other))

    def l2_copy(k, m):
        ref = nb.at[from_o(k), from_h(m) * LO + l]
        return rcopy(ref, ref, ls2.at[k, m], lr2.at[k, m], dev(o, h, other))

    def s1_copy(k):
        return rcopy(s1.at[k], r1.at[k], q1s.at[k], q1r.at[k], dev(o, h, other))

    def s2_copy(k, m):
        return rcopy(s2.at[k, m], r2.at[k, m], q2s.at[k, m], q2r.at[k, m], dev(o, at_h(m), l))

    def s3_copy(k):
        return rcopy(s3.at[k], r3.at[k], q3s.at[k], q3r.at[k], dev(from_o(k), h, l))

    for k in range(1, outer):
        z_copy(k).start()

    def forward(k):
        for m in range(1, hi):
            h_copy(k, m).start()
        l_copy(k).start()

    forward(0)
    for k in range(2, outer):
        wz_copy(k).wait_recv()
        for j in range(1, inner):
            wx_copy(k, j).start()
    own_down.wait()
    for j in range(1, inner):
        for p in range(2):
            wd_copy(j, p).wait_recv()
        for k in range(outer):
            wx_copy(k, j).wait_recv()

    def body(j, carry):
        @pl.when(j + 1 < outer)
        def _():
            z_copy(j + 1).wait_recv()
            forward(j + 1)

        @pl.when(j < outer)
        def _():
            for m in range(1, hi):
                h_copy(j, m).wait_recv()
                l2_copy(j, m).start()
            l_copy(j).wait_recv()
            for m in range(1, hi):
                l2_copy(j, m).wait_recv()
            x = nb[from_o(j)].reshape(tp_size * rows, depth)
            lifted = jnp.dot(x, upbuf[...].reshape(depth, width), preferred_element_type=jnp.float32)
            hidden = jnp.square(jnp.maximum(lifted, 0.0)).astype(jnp.bfloat16)
            part = jnp.dot(hidden, downbuf[...].reshape(width, depth), preferred_element_type=jnp.float32)
            pbuf[...] = part.reshape(tp_size, rows, depth)
            for hh in range(hi):
                s1[j, hh] = pbuf[hh * LO + other].astype(jnp.bfloat16)
            s1_copy(j).start()
            for hh in range(hi):
                acc[j, hh] = pbuf[hh * LO + l]

        @pl.when((j >= 1) & (j < outer + 1))
        def _():
            k = j - 1
            s1_copy(k).wait_recv()
            for m in range(1, hi):
                to = at_h(m)
                s2[k, m] = (acc[k, to] + r1[k, to].astype(jnp.float32)).astype(jnp.bfloat16)
                s2_copy(k, m).start()
            acc2[k] = acc[k, h] + r1[k, h].astype(jnp.float32)

        @pl.when(j >= 2)
        def _():
            k = j - 2
            v = acc2[k]
            for m in range(1, hi):
                s2_copy(k, m).wait_recv()
                v = v + r2[k, m].astype(jnp.float32)
            @pl.when(k == 0)
            def _():
                acc2[0] = v

            @pl.when(k > 0)
            def _():
                s3[k] = v.astype(jnp.bfloat16)
                s3_copy(k).start()

        return carry

    lax.fori_loop(0, outer + 2, body, 0)
    final = stream[...] + acc2[0]
    for k in range(1, outer):
        s3_copy(k).wait_recv()
        final = final + r3[k].astype(jnp.float32)
    out_ref[...] = final.astype(jnp.bfloat16)

    for k in range(1, outer):
        wz_copy(k).wait_send()
        os_copy(k).wait_send()
        ot_copy(k).wait_send()
    for j in range(1, inner):
        for p in range(2):
            wd_copy(j, p).wait_send()
        is_copy(j).wait_send()
        it_copy(j).wait_send()
        for k in range(outer):
            wx_copy(k, j).wait_send()
    c5.wait_send()
    for c in c6:
        c.wait_send()
    for k in range(outer):
        if k > 0:
            z_copy(k).wait_send()
            s3_copy(k).wait_send()
        l_copy(k).wait_send()
        s1_copy(k).wait_send()
        for m in range(1, hi):
            h_copy(k, m).wait_send()
            l2_copy(k, m).wait_send()
            s2_copy(k, m).wait_send()


def on_device(
    sp_size, tp_size,
    query, forget_logits, written_values, output_gate_logits, forget_floor_gap,
    extra_log_decay, head_norm_gain, output_weight, residual, mixer_norm_gain,
    mixer_up_weight, mixer_down_weight,
):
    rows, depth = residual.shape
    length, wide = query.shape
    heads = wide // HEAD_K
    hi = tp_size // LO
    f32, b16 = jnp.float32, jnp.bfloat16
    dma = pltpu.SemaphoreType.DMA
    vm = pltpu.VMEM
    O = OUTER
    inner = sp_size // O
    part, cols = mixer_up_weight.shape
    width = cols // O
    return pl.pallas_call(
        functools.partial(layer_kernel, sp_size, tp_size),
        out_shape=jax.ShapeDtypeStruct((rows, depth), b16),
        in_specs=[pl.BlockSpec(memory_space=pltpu.VMEM)] * 12,
        out_specs=pl.BlockSpec(memory_space=pltpu.VMEM),
        scratch_shapes=[
            vm((sp_size, part, width), b16), vm((inner,) + mixer_down_weight.shape, b16),
            vm((length, wide), f32), vm((length, wide), f32), vm((length, wide), b16),
            vm((inner, heads, HEAD_V, HEAD_K), b16), vm((inner, 8, wide), f32),
            vm((O, heads, HEAD_V, HEAD_K), b16), vm((O, 8, wide), f32),
            vm((tp_size, rows, depth), f32),
            vm((rows, depth), f32),
            vm((hi, rows, depth), b16), vm((hi, rows, depth), b16),
            vm((hi, rows, depth), b16), vm((hi, rows, depth), b16),
            vm((O, tp_size, rows, depth), b16),
            vm((O, hi, rows, depth), f32),
            vm((O, hi, rows, depth), b16), vm((O, hi, rows, depth), b16),
            vm((O, hi, rows, depth), b16), vm((O, hi, rows, depth), b16),
            vm((O, rows, depth), f32),
            vm((O, rows, depth), b16), vm((O, rows, depth), b16),
            dma, dma, dma((hi,)), dma((hi,)),
            dma((O,)), dma((O,)), dma((O, hi)), dma((O, hi)),
            dma((O,)), dma((O,)), dma((O, hi)), dma((O, hi)),
            dma((O,)), dma((O,)), dma((O, hi)), dma((O, hi)),
            dma((O,)), dma((O,)),
            dma((2,)), dma((O,)), dma((O,)), dma((O, inner)), dma((O, inner)),
            dma((inner, 2)), dma((inner, 2)),
            dma((inner,)), dma((inner,)), dma((inner,)), dma((inner,)),
            dma((O,)), dma((O,)), dma((O,)), dma((O,)),
        ],
        compiler_params=pltpu.CompilerParams(
            collective_id=0, has_side_effects=True, vmem_limit_bytes=60 * 1024 * 1024
        ),
    )(
        query, forget_logits, written_values, output_gate_logits,
        forget_floor_gap.reshape(1, wide), extra_log_decay, head_norm_gain.reshape(1, HEAD_V),
        output_weight, residual, mixer_norm_gain.reshape(1, depth),
        mixer_up_weight, mixer_down_weight,
    )


def solution(mesh):
    return jax.shard_map(
        functools.partial(on_device, mesh.shape["sp"], mesh.shape["tp"]),
        mesh=mesh,
        in_specs=(
            P("sp", "tp"),
            P("sp", "tp"),
            P("sp", "tp"),
            P("sp", "tp"),
            P("tp"),
            P("sp", "tp"),
            P(),
            P("tp", None),
            P(("sp", "tp"), None),
            P(),
            P("sp", "tp"),
            P(("tp", "sp"), None),
        ),
        out_specs=P(("sp", "tp"), None),
        check_vma=False,
    )
```
